256 devices in a mesh: ep: 16 (over y, x), tp: 16 (over z, core).
Axes of the slice: x: 4, y: 4, z: 8, core: 2. Of those that a mesh axis runs over, the one named last changes fastest.
Arguments:
- tokens: bfloat16 [1024, 2048], P('ep', 'tp'), may hold values from -6 to 6
- norm_gain: float32 [2048], replicated, may hold values from 0.5 to 1.5
- group_pick: int32 [1024, 1], P('ep'), may hold values from 0 to 15; in each aligned block of 64 rows (0 to 63, 64 to 127, ...) at most 18 rows name the same one
- inner_pick: int32 [1024, 2], P('ep'), may hold values from 0 to 3, all different within a row
- route_weight: float32 [1024, 2], P('ep'), may hold values from 0.3 to 1
- w_gate: bfloat16 [64, 1024, 2048], P('ep', 'tp'), may hold values from -0.125 to 0.125
- w_up: bfloat16 [64, 1024, 2048], P('ep', 'tp'), may hold values from -0.125 to 0.125
- w_down: bfloat16 [64, 1024, 2048], P('ep', 'tp'), may hold values from -0.1875 to 0.1875
Outputs:
- mixed: bfloat16 [1024, 2048], P('ep', 'tp')
The draws below stay inside these ranges and needn't reach their ends.
Inputs may be any that keep to these rules, and one draw needn't show every extreme that they name: `group_pick`: every entry is a group, 0 to 15; among the 64 tokens of any one index of ep no group is chosen more than 18 times, a bound that some block reaches. `inner_pick`: each row names 2 different experts of the chosen group, each 0 to 3.
All inputs are finite; a program needn't handle non-finite values.
Results may differ from the reference program's by a relative error of at most 0.002.
Values may be sent and summed in bfloat16 or wider, within the bound.
A program may use at most 64 MiB of HBM per device.

```python
import math
import jax
import jax.numpy as jnp
import numpy as np
from jax import lax

D = 2048
FF = 1024
EXP_GROUP = 4
TOP = 2
TOK_DEV = 64
GROUPS = 16
EXPERTS = 64
TOKENS = 1024
CAP = 18


def levels(key, dims, pieces, low, largest):
    def one(dim, shards_of):
        heights = jax.random.uniform(jax.random.fold_in(jax.random.fold_in(key, 6), dim), (shards_of,), jnp.float32, low / len(pieces), largest / len(pieces))
        return jnp.repeat(jnp.exp(heights), dims[dim] // shards_of).reshape((-1,) + (1,) * (len(dims) - dim - 1))

    gain = one(*pieces[0])
    for cut in pieces[1:]:
        gain = gain * one(*cut)
    return gain


def choose_distinct(rng, rows, number_of, top, lift):
    sequence = jax.random.permutation(jax.random.fold_in(rng, 1), number_of)
    favour = sequence
    for power in range(3):
        favour = favour * favour // number_of
    favour = favour * lift // number_of
    chance = jax.random.randint(jax.random.fold_in(rng, 2), (rows, number_of), 0, 4096) + favour
    fixed_rows = jax.random.permutation(jax.random.fold_in(rng, 3), rows)[jnp.arange(number_of) % rows]
    chance = jnp.where(jnp.arange(rows)[:, None] == fixed_rows[None, :], 1 << 14, chance)
    merit = chance * number_of + jnp.arange(number_of)
    return lax.top_k(merit.astype(jnp.int32), top)[1].astype(jnp.int32)


def shared_out(rng, own, number, rows, count, top, most, slope):
    ranking = jax.random.permutation(rng, count)
    crowded, common = load_shares(count, rows * top, most, slope, True), load_shares(count, rows * top, most, slope, False)
    places = jnp.arange(count)

    def named(sizes, offset_by):
        used = int((sizes > 0).sum())
        fixed = max(1, used // 4)
        passed = fixed + (places - fixed + offset_by * (used - fixed)) % max(1, count - fixed)
        return jnp.zeros((count,), jnp.int32).at[ranking[jnp.where(places < fixed, places, passed)]].set(jnp.asarray(sizes, jnp.int32))

    sizes = jnp.where(number % 4 == 0, named(crowded, number // 4), named(common, number - number // 4 - 1))
    mixed = jax.random.permutation(jax.random.fold_in(own, 3), count)
    donor, taker = mixed[0:count // 2 * 2:2], mixed[1:count // 2 * 2:2]
    room = jnp.minimum(sizes[donor] - 1, most - sizes[taker]) // 2
    room = jnp.where((donor == ranking[0]) | (taker == ranking[0]) | (sizes[taker] == 0), 0, jnp.maximum(room, 0))
    passed = jax.random.randint(jax.random.fold_in(own, 4), (count // 2,), 0, 1 << 20) % (room + 1)
    sizes = sizes.at[donor].add(-passed).at[taker].add(passed)
    members = jnp.searchsorted(jnp.cumsum(sizes), jnp.arange(rows * top), side="right").astype(jnp.int32)
    table = members.reshape(top, rows).T
    table = table[jax.random.permutation(jax.random.fold_in(own, 1), rows)]
    offset_by = jax.random.randint(jax.random.fold_in(own, 2), (rows, 1), 0, top)
    return jnp.take_along_axis(table, (jnp.arange(top)[None, :] + offset_by) % top, axis=1)


def load_shares(amount, total, limit, skew, full):
    loads = [(1 << 20) // math.isqrt(rank ** skew) + 1 for rank in range(1, amount + 1)]
    largest = limit if full else min(limit, max(-(-total // amount), total * loads[0] // sum(loads)))
    least = 1 if total - largest >= amount - 1 else 0
    given, spare = [largest] + [least] * (amount - 1), total - largest - least * (amount - 1)
    while spare > 0:
        candidates = [i for i in range(1, amount) if given[i] < largest] or [i for i in range(1, amount) if given[i] < limit]
        pool, remaining = sum([loads[i] for i in candidates]), spare
        for i in candidates:
            addition = min(limit - given[i], max(1, remaining * loads[i] // pool), spare)
            given[i] = given[i] + addition
            spare = spare - addition
    return np.array(given)


def bell_draw(own_key, extent, scale, bound, cuts=(), kind=jnp.bfloat16):
    result = jax.random.normal(own_key, extent, jnp.float32) * scale
    if len(cuts) > 0:
        result = levels(own_key, extent, cuts, -0.22, 0.18) * result
    return jnp.clip(result, min=-bound, max=bound).astype(kind)


def setup_inputs(seed: int = 0) -> dict:
    splits = jax.random.split(jax.random.key(seed), 9)
    tokens = bell_draw(splits[0], (TOKENS, D), 1.0, 6.0, ((0, 16), (1, 16)))
    norm_gain = jnp.clip(1.0 + 0.1 * jax.random.normal(splits[1], (D,), jnp.float32), 0.5, 1.5)
    group_pick_keys = jax.random.split(jax.random.fold_in(splits[2], 1), TOKENS // TOK_DEV)
    group_pick_turns = jax.random.permutation(jax.random.fold_in(splits[2], 3), TOKENS // TOK_DEV)
    group_pick = jax.vmap(lambda own, number: shared_out(jax.random.fold_in(splits[2], 2), own, number, TOK_DEV, GROUPS, 1, CAP, 2))(group_pick_keys, group_pick_turns).reshape((TOKENS, 1))
    inner_pick = choose_distinct(splits[3], TOKENS, EXP_GROUP, TOP, 0)
    route_weight = jnp.clip(0.3 + 0.7 * jax.random.uniform(splits[4], (TOKENS, TOP), jnp.float32) ** levels(splits[4], (TOKENS, TOP), ((0, 16),), -0.2, 0.2), 0.3, 1.0)
    w_gate = bell_draw(splits[5], (EXPERTS, FF, D), D ** -0.5, 0.125, ((0, 16), (1, 16)))
    w_up = bell_draw(splits[6], (EXPERTS, FF, D), D ** -0.5, 0.125, ((0, 16), (1, 16)))
    w_down = bell_draw(splits[7], (EXPERTS, FF, D), FF ** -0.5, 0.1875, ((0, 16), (1, 16)))
    return dict(tokens=tokens, norm_gain=norm_gain, group_pick=group_pick, inner_pick=inner_pick, route_weight=route_weight, w_gate=w_gate, w_up=w_up, w_down=w_down)


epsilon = 1e-06

def reference(tokens, norm_gain, group_pick, inner_pick, route_weight, w_gate, w_up, w_down):
    widened = tokens.astype(jnp.float32)
    scaled = lax.rsqrt(lax.optimization_barrier(jnp.mean(widened * widened, axis=-1, keepdims=True)) + epsilon)
    normed = (widened * scaled * norm_gain).astype(jnp.bfloat16)
    chosen = (group_pick * EXP_GROUP + inner_pick).astype(jnp.int32)

    def one_token(packed):
        token_row, token_picks, token_weights = packed
        running = jnp.zeros((D,), jnp.float32)
        for ordinal in range(TOP):
            expert = token_picks[ordinal]
            gate_proj = jnp.dot(w_gate[expert], token_row, preferred_element_type=jnp.float32)
            up_proj = jnp.dot(w_up[expert], token_row, preferred_element_type=jnp.float32)
            hidden = (jax.nn.silu(gate_proj) * up_proj).astype(jnp.bfloat16)
            product = jnp.dot(hidden, w_down[expert], preferred_element_type=jnp.float32)
            running = running + token_weights[ordinal] * product
        return running
    mixed_rows = lax.map(one_token, (normed, chosen, route_weight))
    return mixed_rows.astype(jnp.bfloat16)
```

```python
import functools

import jax
import jax.numpy as jnp
from jax import lax
from jax.experimental import pallas as pl
from jax.experimental.pallas import tpu as pltpu
from jax.sharding import PartitionSpec as P

MESH = pl.DeviceIdType.MESH
EPS = 1e-06
EP = 16
SIDE = 4
TP = 16
RING = 8
SLOTS = 18
PAD = 32
ROWS = EP * SLOTS
HALF = ROWS // 2
LANES = 128
F32 = jnp.float32
BF16 = jnp.bfloat16


def iota(shape, dim):
    return lax.broadcasted_iota(jnp.int32, shape, dim)


def one_hot(mask):
    return jnp.where(mask, 1.0, 0.0).astype(BF16)


def dot(a, b, dims=((1,), (0,))):
    return lax.dot_general(a, b, (dims, ((), ())), preferred_element_type=F32)


NT = ((1,), (1,))
TN = ((0,), (0,))


def kernel(
    tokens_ref, gain_ref, group_ref, inner_ref, weight_ref, w_gate_ref, w_up_ref, w_down_ref,
    out_ref,
    wgu_ref, wd_ref, place_ref, send_ref, recv_ref, tr_ref, gates_ref, x_ref, normed_ref, hl_ref,
    own_ref, give_ref, take_ref, sp_ref, sm_ref, rp_ref, rm_ref, back_ref, home_ref,
    w_sem, d_send, d_recv, agp_send, agp_recv, agm_send, agm_recv, agx_send, agx_recv,
    rx_send, rx_recv, rp_send, rp_recv, rm_send, rm_recv, h_send, h_recv,
):
    ep = lax.axis_index("ep")
    tp = lax.axis_index("tp")
    ey, ex = ep // SIDE, ep % SIDE
    z, core = tp // 2, tp % 2
    up = (tp + 2) % TP
    down = (tp + TP - 2) % TP
    partner = z * 2 + (1 - core)
    steps = [(dy, dx) for dy in range(SIDE) for dx in range(SIDE) if dy or dx]
    steps.sort(key=lambda s: -(min(s[0], SIDE - s[0]) + min(s[1], SIDE - s[1])))

    def peer(dy, dx):
        return ((ey + dy) % SIDE) * SIDE + (ex + dx) % SIDE

    barrier = pltpu.get_barrier_semaphore()
    for dy, dx in steps:
        pl.semaphore_signal(barrier, inc=1, device_id={"ep": peer(dy, dx)}, device_id_type=MESH)
    for to in (up, down, partner):
        pl.semaphore_signal(barrier, inc=1, device_id={"tp": to}, device_id_type=MESH)

    experts = w_gate_ref.shape[0]
    loads = [
        pltpu.make_async_copy(w_gate_ref, wgu_ref.at[pl.ds(0, experts)], w_sem.at[0]),
        pltpu.make_async_copy(w_up_ref, wgu_ref.at[pl.ds(experts, experts)], w_sem.at[1]),
        pltpu.make_async_copy(w_down_ref, wd_ref, w_sem.at[2]),
    ]
    for load in loads:
        load.start()

    toks = tokens_ref.shape[0]
    groups = group_ref[...]
    member = one_hot(iota((EP, toks), 0) == groups)
    before = one_hot(iota((toks, toks), 0) < iota((toks, toks), 1))
    earlier = dot(member, before)
    earlier = jnp.sum(earlier * member.astype(F32), axis=0, keepdims=True)
    position = groups * PAD + earlier.astype(jnp.int32)
    place_ref[...] = one_hot(iota((EP * PAD, toks), 0) == position)
    placing = place_ref[...]
    packed = dot(placing, tokens_ref[...]).reshape(EP, PAD, LANES)
    row = iota((16, toks), 0)
    expert = jnp.where(row >= 5, 1, 0) + jnp.where(row >= 8, 1, 0) + jnp.where(row >= 11, 1, 0)
    part = row - 2 - 3 * expert
    gate = jnp.where(inner_ref[0:1, :] == expert, weight_ref[0:1, :], 0.0) + jnp.where(
        inner_ref[1:2, :] == expert, weight_ref[1:2, :], 0.0
    )
    first = gate.astype(BF16).astype(F32)
    second = (gate - first).astype(BF16).astype(F32)
    third = gate - first - second
    parts = jnp.where(part == 0, first, jnp.where(part == 1, second, third))
    parts = jnp.where((row >= 2) & (row < 14), parts, 0.0).astype(BF16)
    parts = dot(parts, placing, NT)
    for g in range(EP):
        col = (g * PAD) // LANES * LANES
        send_ref[g, 0:16] = packed[g, 0:16].astype(BF16)
        send_ref[g, 16:32] = (packed[g, 16:32] + parts[:, col : col + LANES]).astype(BF16)

    pl.semaphore_wait(barrier, len(steps) + 3)

    sends = []
    for i, (dy, dx) in enumerate(steps):
        to = peer(dy, dx)
        sends.append(
            pltpu.make_async_remote_copy(
                send_ref.at[to], recv_ref.at[ep], d_send.at[i], d_recv.at[i],
                device_id={"ep": to}, device_id_type=MESH,
            )
        )
        sends[-1].start()
    recv_ref[ep] = send_ref[ep]
    for copy in reversed(sends):
        copy.wait_recv()

    r_col = iota((ROWS, 1), 0)
    src_col = (r_col * 3641) >> 16
    slot_col = r_col - src_col * SLOTS
    pick = one_hot(iota((ROWS, EP * PAD), 1) == src_col * PAD + slot_col)
    x_ref[tp] = dot(pick, recv_ref[...].reshape(EP * PAD, LANES)).astype(BF16)

    def ring(buf_at, send, recv, to):
        return pltpu.make_async_remote_copy(
            buf_at, buf_at, send, recv, device_id={"tp": to}, device_id_type=MESH
        )

    def piece(z_of, of_core, half):
        at = x_ref.at[z_of * 2 + of_core]
        if half is not None:
            at = at.at[pl.ds(half * HALF, HALF)]
        return at

    gp, gm, gx = [], [], []
    for i, half in enumerate((0, 1)):
        gp.append(ring(piece(z, core, half), agp_send.at[i], agp_recv.at[i], up))
        gp[-1].start()
        gm.append(ring(piece(z, core, 1 - half), agm_send.at[i], agm_recv.at[i], down))
        gm[-1].start()
    gx.append(ring(piece(z, core, None), agx_send.at[0], agx_recv.at[0], partner))
    gx[-1].start()

    tr_ref[...] = jnp.transpose(recv_ref[:, 16:32, :].astype(F32).reshape(EP * 16, LANES))
    near = tr_ref[pl.ds(pl.multiple_of((ep % 4) * PAD, PAD), PAD), :].astype(BF16)
    chosen = dot(one_hot(iota((ROWS, PAD), 1) == slot_col), near)
    lane = iota((ROWS, EP * 16), 1)
    chosen = jnp.where(lane >> 4 == src_col, chosen, 0.0).astype(BF16)
    units = w_gate_ref.shape[1]
    which = iota((EP * 16, experts * units), 0) & 15
    owner = iota((EP * 16, experts * units), 1) >> 6
    spread = one_hot((which >= 2 + 3 * owner) & (which < 5 + 3 * owner))
    gates_ref[...] = dot(chosen, spread)

    def squares(t, half):
        if half is None:
            v = x_ref[t].astype(F32)
        else:
            v = x_ref[t, half * HALF : (half + 1) * HALF].astype(F32)
        return v * v

    total = squares(tp, None)
    own_ref[0] = total
    for s in range(4):
        for i in range(2 if s < 3 else 1):
            for sign, copies, send, recv, to in (
                (-1, gp, agp_send, agp_recv, up),
                (1, gm, agm_send, agm_recv, down),
            ):
                half = i if sign < 0 else 1 - i
                z_of = (z + sign * (1 + s) + RING) % RING
                k = 2 * s + i
                ring(piece(z_of, core, half), send.at[k], recv.at[k], to).wait_recv()
                if s < 2 or (s == 2 and i == 0):
                    copies.append(ring(piece(z_of, core, half), send.at[k + 2], recv.at[k + 2], to))
                    copies[-1].start()
                n = len(gx)
                gx.append(ring(piece(z_of, core, half), agx_send.at[n], agx_recv.at[n], partner))
                gx[-1].start()
                at = pl.ds(half * HALF, HALF)
                own_ref[0, at] = own_ref[0, at] + squares(z_of * 2 + core, half)
    for copy in gx:
        copy.wait_recv()
    total = own_ref[0]
    for zz in range(RING):
        total = total + squares(zz * 2 + (1 - core), None)
    scale = lax.rsqrt(jnp.sum(total, axis=1, keepdims=True) * (1.0 / (TP * LANES)) + EPS)
    for t in range(TP):
        cols = slice(t * LANES, (t + 1) * LANES)
        normed_ref[:, cols] = (x_ref[t].astype(F32) * scale * gain_ref[:, cols]).astype(BF16)

    for load in loads:
        load.wait()
    width = experts * units
    proj = dot(normed_ref[...], wgu_ref[...].reshape(2 * width, TP * LANES), NT)
    gate_proj, up_proj = proj[:, :width], proj[:, width:]
    hidden = (gate_proj / (1.0 + jnp.exp(-gate_proj)) * up_proj).astype(BF16).astype(F32)
    gated = hidden * gates_ref[...]
    high = gated.astype(BF16)
    hl_ref[0] = high
    hl_ref[1] = (gated - high.astype(F32)).astype(BF16)

    rx = []

    def partial(offset):
        k = len(rx)
        z_of = (z + offset + RING) % RING
        cols = pl.ds(pl.multiple_of(z_of * 2 * LANES, 2 * LANES), 2 * LANES)
        w = wd_ref[:, :, cols].reshape(width, 2 * LANES)
        both = dot(hl_ref[0], w) + dot(hl_ref[1], w)
        own_ref[k] = jnp.where(core == 0, both[:, :LANES], both[:, LANES:])
        give_ref[k] = jnp.where(core == 0, both[:, LANES:], both[:, :LANES])
        rx.append(
            pltpu.make_async_remote_copy(
                give_ref.at[k], take_ref.at[k], rx_send.at[k], rx_recv.at[k],
                device_id={"tp": partner}, device_id_type=MESH,
            )
        )
        rx[-1].start()

    def mine(k, half):
        at = slice(half * HALF, (half + 1) * HALF)
        return own_ref[k, at] + take_ref[k, at]

    sp, sm = {}, {}

    def pass_on(copies, k, value, src, dst, send, recv, to):
        src[k] = value
        copies[k] = pltpu.make_async_remote_copy(
            src.at[k], dst.at[k], send.at[k], recv.at[k], device_id={"tp": to}, device_id_type=MESH
        )
        copies[k].start()

    def pass_up(k, value):
        pass_on(sp, k, value, sp_ref, rp_ref, rp_send, rp_recv, up)

    def pass_down(k, value):
        pass_on(sm, k, value, sm_ref, rm_ref, rm_send, rm_recv, down)

    partial(4)
    partial(3)
    partial(-3)
    rx[0].wait_recv()
    pass_up(0, mine(0, 0))
    pass_down(0, mine(0, 1))
    rx[1].wait_recv()
    pass_up(1, mine(1, 1))
    rx[2].wait_recv()
    pass_down(1, mine(2, 0))
    partial(2)
    partial(-2)
    sp[0].wait_recv()
    pass_up(2, mine(1, 0) + rp_ref[0])
    sm[0].wait_recv()
    pass_down(2, mine(2, 1) + rm_ref[0])
    partial(1)
    partial(-1)
    partial(0)
    rx[3].wait_recv()
    sp[1].wait_recv()
    pass_up(3, mine(3, 1) + rp_ref[1])
    rx[4].wait_recv()
    sm[1].wait_recv()
    pass_down(3, mine(4, 0) + rm_ref[1])
    sp[2].wait_recv()
    pass_up(4, mine(3, 0) + rp_ref[2])
    sm[2].wait_recv()
    pass_down(4, mine(4, 1) + rm_ref[2])
    rx[5].wait_recv()
    sp[3].wait_recv()
    pass_up(5, mine(5, 1) + rp_ref[3])
    rx[6].wait_recv()
    sm[3].wait_recv()
    pass_down(5, mine(6, 0) + rm_ref[3])
    sp[4].wait_recv()
    pass_up(6, mine(5, 0) + rp_ref[4])
    sm[4].wait_recv()
    pass_down(6, mine(6, 1) + rm_ref[4])
    rx[7].wait_recv()
    sp[5].wait_recv()
    sm[5].wait_recv()
    sp[6].wait_recv()
    sm[6].wait_recv()
    upper = mine(7, 0) + rp_ref[6] + rm_ref[5]
    lower = mine(7, 1) + rp_ref[5] + rm_ref[6]

    r_row = iota((1, ROWS), 1)
    src_row = (r_row * 3641) >> 16
    target = src_row * PAD + (r_row - src_row * SLOTS)
    unpick = one_hot(iota((EP * PAD, ROWS), 0) == target)
    summed = jnp.concatenate([upper, lower], axis=0).astype(BF16)
    back_ref[...] = dot(unpick, summed).astype(BF16).reshape(EP, PAD, LANES)
    returns = []
    for i, (dy, dx) in enumerate(steps):
        to = peer(dy, dx)
        returns.append(
            pltpu.make_async_remote_copy(
                back_ref.at[to], home_ref.at[ep], h_send.at[i], h_recv.at[i],
                device_id={"ep": to}, device_id_type=MESH,
            )
        )
        returns[-1].start()
    home_ref[ep] = back_ref[ep]
    for copy in reversed(returns):
        copy.wait_recv()
    home = home_ref[...].reshape(EP * PAD, LANES)
    out_ref[...] = dot(place_ref[...], home, TN).astype(BF16)

    for copy in sends + gp + gm + gx + rx + list(sp.values()) + list(sm.values()) + returns:
        copy.wait_send()


def per_device(tokens, norm_gain, group_pick, inner_pick, route_weight, w_gate, w_up, w_down):
    toks = tokens.shape[0]
    experts, units, model = w_gate.shape
    width = experts * units
    vmem = pl.BlockSpec(memory_space=pltpu.VMEM)
    hbm = pl.BlockSpec(memory_space=pl.ANY)
    dma = pltpu.SemaphoreType.DMA
    return pl.pallas_call(
        kernel,
        name="moe_step",
        out_shape=jax.ShapeDtypeStruct(tokens.shape, BF16),
        in_specs=[vmem] * 5 + [hbm] * 3,
        out_specs=vmem,
        scratch_shapes=[
            pltpu.VMEM((2 * experts, units, model), BF16),
            pltpu.VMEM((experts, units, model), BF16),
            pltpu.VMEM((EP * PAD, toks), BF16),
            pltpu.VMEM((EP, PAD, LANES), BF16),
            pltpu.VMEM((EP, PAD, LANES), BF16),
            pltpu.VMEM((LANES, EP * 16), F32),
            pltpu.VMEM((ROWS, width), F32),
            pltpu.VMEM((TP, ROWS, LANES), BF16),
            pltpu.VMEM((ROWS, model), BF16),
            pltpu.VMEM((2, ROWS, width), BF16),
            pltpu.VMEM((8, ROWS, LANES), F32),
            pltpu.VMEM((8, ROWS, LANES), F32),
            pltpu.VMEM((8, ROWS, LANES), F32),
            pltpu.VMEM((7, HALF, LANES), F32),
            pltpu.VMEM((7, HALF, LANES), F32),
            pltpu.VMEM((7, HALF, LANES), F32),
            pltpu.VMEM((7, HALF, LANES), F32),
            pltpu.VMEM((EP, PAD, LANES), BF16),
            pltpu.VMEM((EP, PAD, LANES), BF16),
            dma((3,)),
            dma((15,)), dma((15,)),
            dma((7,)), dma((7,)), dma((7,)), dma((7,)),
            dma((15,)), dma((15,)),
            dma((8,)), dma((8,)),
            dma((7,)), dma((7,)), dma((7,)), dma((7,)),
            dma((15,)), dma((15,)),
        ],
        compiler_params=pltpu.CompilerParams(
            collective_id=0, has_side_effects=True, vmem_limit_bytes=48 * 1024 * 1024
        ),
    )(
        tokens, norm_gain.reshape(1, model), group_pick.T, inner_pick.T, route_weight.T,
        w_gate, w_up, w_down,
    )


def solution(mesh):
    return jax.shard_map(
        per_device,
        mesh=mesh,
        in_specs=(
            P("ep", "tp"),
            P(),
            P("ep", None),
            P("ep", None),
            P("ep", None),
            P("ep", "tp", None),
            P("ep", "tp", None),
            P("ep", "tp", None),
        ),
        out_specs=P("ep", "tp"),
        check_vma=False,
    )
```
